32 devices in a mesh: fs: 8 (over z, x), tp: 4 (over y, core).
Axes of the slice: x: 2, y: 2, z: 4, core: 2. Of those that a mesh axis runs over, the one named last changes fastest.
Arguments:
- normed_input: bfloat16 [16384, 2048], P('fs'), may hold values from -6 to 6
- output_cotangent: bfloat16 [16384, 2048], P('fs'), may hold values from -6 to 6
- query_grad: bfloat16 [16384, 2048], P('fs', 'tp'), may hold values from -0.75 to 0.75
- key_grad: bfloat16 [16384, 2048], P('fs', 'tp'), may hold values from -0.75 to 0.75
- attn_values: bfloat16 [16384, 2048], P('fs', 'tp'), may hold values from -0.75 to 0.75
- master_weights: float32 [3, 2048, 2048], P(None, 'fs', 'tp'), may hold values from -3 to 3
- factors: bfloat16 [3, 2048, 256], P(None, 'fs'), may hold values from -0.375 to 0.375
- moments: float32 [3, 256, 2048], P(None, 'fs', 'tp'), may hold values from -620 to 620
Outputs:
- new_weights: float32 [3, 2048, 2048], P(None, 'fs', 'tp')
- weight_copies: bfloat16 [3, 2048, 2048], P(None, None, 'tp')
- steps: float32 [3, 2048, 2048], P(None, 'fs', 'tp')
- new_moments: float32 [3, 256, 2048], P(None, 'fs', 'tp')
The draws below stay inside these ranges and needn't reach their ends.
All inputs are finite; a program needn't handle non-finite values.
Results may differ from the reference program's by a relative error of at most 0.0055.
Values may be sent and summed in bfloat16 or wider, within the bound.
A program may use at most 128 MiB of HBM per device.

```python
import jax
import jax.numpy as jnp
from jax import lax

D = 2048
RANK = 256
TOKENS = 16384


def column_law(key, rows, cols):
    first, second = jax.random.split(key)
    column = jnp.arange(cols, dtype=jnp.float32)
    rough = jax.random.uniform(second, (cols,), jnp.float32, 0.6, 1.6)
    scale = 10.0 ** (column / max(cols - 1, 1)) * rough
    base = jnp.clip(jax.random.normal(first, (rows, cols), jnp.float32), -6.0, 6.0)
    return base * scale[None, :]


def draw_query_grad(key, part):
    return (column_law(jax.random.fold_in(key, 11), TOKENS, D) * TOKENS ** (-0.5)).astype(jnp.bfloat16)


def draw_key_grad(key, part):
    return (column_law(jax.random.fold_in(key, 12), TOKENS, D) * TOKENS ** (-0.5)).astype(jnp.bfloat16)


def draw_attn_values(key, part):
    return (column_law(jax.random.fold_in(key, 13), TOKENS, D) * TOKENS ** (-0.5)).astype(jnp.bfloat16)


def draw_moments(key, part):
    blocks = []
    for index in range(3):
        inner = jax.random.fold_in(key, 20 + index)
        values = column_law(inner, RANK, D)
        row = jnp.arange(RANK, dtype=jnp.float32)
        lift = 10.0 ** (0.5 * row / max(RANK - 1, 1))
        blocks.append(2.0 * values * lift[:, None])
    return jnp.stack(blocks).astype(jnp.float32)


def block_levels(rng, dims, cuts, low, top_value):
    def one(axis_at, shards_of):
        steps = jax.random.uniform(jax.random.fold_in(jax.random.fold_in(rng, 6), axis_at), (shards_of,), jnp.float32, low / len(cuts), top_value / len(cuts))
        return jnp.repeat(jnp.exp(steps), dims[axis_at] // shards_of).reshape((-1,) + (1,) * (len(dims) - axis_at - 1))

    loudness = one(*cuts[0])
    for cut in cuts[1:]:
        loudness = loudness * one(*cut)
    return loudness


def centred(stream_key, dims, width, reach, cuts=(), kind=jnp.bfloat16):
    result = jax.random.normal(stream_key, dims, jnp.float32) * width
    if len(cuts) > 0:
        result = block_levels(stream_key, dims, cuts, -0.22, 0.18) * result
    return jnp.clip(result, min=-reach, max=reach).astype(kind)


def setup_inputs(seed: int = 0) -> dict:
    arg_keys = jax.random.split(jax.random.key(seed), 9)
    return {
        "normed_input": centred(arg_keys[0], (TOKENS, D), 1.0, 6.0, ((0, 8),)),
        "output_cotangent": centred(arg_keys[1], (TOKENS, D), 1.0, 6.0, ((0, 8),)),
        "query_grad": draw_query_grad(jax.random.fold_in(arg_keys[8], 71), 0),
        "key_grad": draw_key_grad(jax.random.fold_in(arg_keys[8], 71), 0),
        "attn_values": draw_attn_values(jax.random.fold_in(arg_keys[8], 71), 0),
        "master_weights": centred(arg_keys[5], (3, D, D), 0.5, 3.0, ((1, 8), (2, 4)), jnp.float32),
        "factors": centred(arg_keys[6], (3, D, RANK), RANK ** -0.5, 0.375, ((1, 8),)),
        "moments": draw_moments(jax.random.fold_in(arg_keys[8], 71), 0),
    }


def reference(normed_input, output_cotangent, query_grad, key_grad, attn_values, master_weights, factors, moments):
    pairs = ((normed_input, query_grad), (normed_input, key_grad), (output_cotangent, attn_values))
    updated = []
    for index in range(3):
        left, right = pairs[index]
        gradient = jnp.dot(left.T, right, preferred_element_type=jnp.float32)
        projected = jnp.dot(factors[index].astype(jnp.float32).T, gradient, precision=lax.Precision.HIGHEST)
        updated.append(0.8 * moments[index] + 0.2 * projected)
    new_moments = jnp.stack(updated)
    rms = jnp.sqrt(jnp.mean(new_moments * new_moments) + 1e-06)
    normalized = (new_moments / rms).astype(jnp.bfloat16)
    steps = jnp.stack([jnp.dot(factors[index], normalized[index], preferred_element_type=jnp.float32) for index in range(3)])
    new_weights = master_weights - 0.05 * steps
    return (new_weights, new_weights.astype(jnp.bfloat16), steps, new_moments)
```

```python
import functools

import jax
import jax.numpy as jnp
from jax import lax
from jax.experimental import pallas as pl
from jax.experimental.pallas import tpu as pltpu
from jax.sharding import PartitionSpec as P

MESH = pl.DeviceIdType.MESH
F32 = jnp.float32
BF16 = jnp.bfloat16


def grid_of(count):
    cols = 1
    while cols * cols * 4 <= count:
        cols *= 2
    return count // cols, cols


class Relay:
    def __init__(self, own, slot, send, recv, first, second, dev, hook=None, hook_drain=None):
        self.own, self.slot, self.send, self.recv = own, slot, send, recv
        (self.a, self.na), (self.b, self.nb) = first, second
        self.dev, self.hook, self.hook_drain = dev, hook, hook_drain
        a, b = self.a, self.b
        self.open = [a + 1 < self.na, a >= 1, b + 1 < self.nb, b >= 1]
        self.target = [(a + 1, b), (a - 1, b), (a, b + 1), (a, b - 1)]
        self.sent = []
        self.steps = [self.start]
        self.steps += [functools.partial(self.along_first, k) for k in range(1, self.na)]
        self.steps += [functools.partial(self.along_second, k) for k in range(1, self.nb)]
        self.at = 0

    def copy(self, owner, way, src):
        return pltpu.make_async_remote_copy(
            src_ref=src,
            dst_ref=self.slot(owner),
            send_sem=self.send.at[owner, way],
            recv_sem=self.recv.at[owner],
            device_id={"fs": self.dev(*self.target[way])},
            device_id_type=MESH,
        )

    def push(self, cond, owner, way, src):
        both = self.open[way] if cond is None else jnp.logical_and(cond, self.open[way])
        self.sent.append((both, owner, way, src))

        @pl.when(both)
        def _():
            self.copy(owner, way, src).start()

    def arrive(self, cond, owner, ways, came):
        @pl.when(cond)
        def _():
            self.copy(owner, came, self.slot(owner)).wait_recv()

        for way in ways:
            self.push(cond, owner, way, self.slot(owner))
        if self.hook is not None:

            @pl.when(cond)
            def _():
                self.hook(owner)

    def start(self):
        me = self.dev(self.a, self.b)
        for way in range(4):
            self.push(None, me, way, self.own)

    def along_first(self, k):
        self.arrive(self.a >= k, self.dev(self.a - k, self.b), (0, 2, 3), 1)
        self.arrive(self.a + k < self.na, self.dev(self.a + k, self.b), (1, 2, 3), 0)

    def along_second(self, k):
        for row in range(self.na):
            self.arrive(self.b >= k, self.dev(row, self.b - k), (2,), 3)
            self.arrive(self.b + k < self.nb, self.dev(row, self.b + k), (3,), 2)

    def tick(self, count=1):
        for _ in range(count):
            if self.at < len(self.steps):
                self.steps[self.at]()
                self.at += 1

    def finish(self):
        self.tick(len(self.steps))

    def drain(self):
        for cond, owner, way, src in self.sent:

            @pl.when(cond)
            def _():
                self.copy(owner, way, src).wait_send()


def exchange_kernel(
    nfs, ntp,
    x_in, o_in, q_in, k_in, v_in, w_in, p_in, m_ref,
    wfull, pfull, nmfull, new_m, total,
    xbuf, ybuf, sacc, sbuf, rbuf, tbuf, ubuf,
    load_sem, p_send, p_recv, d_send, d_recv, w_send, w_recv, n_send, n_recv,
    r_send, r_recv, t_send, t_recv, u_send, u_recv,
):
    me = lax.axis_index("fs")
    tp = lax.axis_index("tp")
    nz, nx = grid_of(nfs)
    z, x = me // nx, me % nx
    core = tp % 2
    mate = tp + 1 - 2 * core
    block = p_in.shape[1]
    half = block // 2
    rr = m_ref.shape[1]

    loads = [
        pltpu.make_async_copy(p_in, pfull.at[:, pl.ds(pl.multiple_of(me * block, block), block), :], load_sem.at[0]),
        pltpu.make_async_copy(x_in, xbuf.at[0], load_sem.at[1]),
        pltpu.make_async_copy(q_in, ybuf.at[0], load_sem.at[2]),
        pltpu.make_async_copy(k_in, ybuf.at[1], load_sem.at[3]),
        pltpu.make_async_copy(o_in, xbuf.at[1], load_sem.at[4]),
        pltpu.make_async_copy(v_in, ybuf.at[2], load_sem.at[5]),
    ]

    def zx(row, col):
        return row * nx + col

    def xz(col, row):
        return row * nx + col

    def p_slot(owner, which):
        return pfull.at[:, pl.ds(pl.multiple_of(owner * block + which * half, half), half), :]

    def mate_copy(owner, which):
        return pltpu.make_async_remote_copy(
            src_ref=p_slot(owner, which),
            dst_ref=p_slot(owner, which),
            send_sem=d_send.at[owner],
            recv_sem=d_recv.at[owner],
            device_id={"tp": mate},
            device_id_type=MESH,
        )

    factors = Relay(
        p_in.at[:, pl.ds(pl.multiple_of(core * half, half), half), :],
        lambda owner: p_slot(owner, core),
        p_send, p_recv, (z, nz), (x, nx), zx,
        hook=lambda owner: mate_copy(owner, core).start(),
    )

    def w_piece(index, j, low, size, across):
        def slot(owner):
            return wfull.at[j, pl.ds(pl.multiple_of(owner * block + low, half), size), :]

        first, second, dev = ((x, nx), (z, nz), xz) if across else ((z, nz), (x, nx), zx)
        return Relay(
            w_in.at[j, pl.ds(low, size), :], slot, w_send.at[index], w_recv.at[index], first, second, dev
        )

    weights = [
        w_piece(0, 0, 0, block, False),
        w_piece(1, 1, 0, block, False),
        w_piece(2, 2, 0, half, False),
        w_piece(3, 2, half, half, True),
    ]

    def n_slot(owner):
        return nmfull.at[:, pl.ds(pl.multiple_of(owner * rr, rr), rr), :]

    momentum = Relay(n_slot(me), n_slot, n_send, n_recv, (z, nz), (x, nx), zx)

    factors.tick()
    for load in loads:
        load.start()
    factors.tick(2)
    weights[0].tick()
    factors.finish()
    weights[0].tick()
    weights[3].tick()
    loads[0].wait()
    for m in range(1, nfs):
        owner = lax.rem(me + m, nfs)
        mate_copy(owner, 1 - core).wait_recv()

    tokens = xbuf.shape[1]
    tile = min(256, tokens)

    def scatter_copy(j, m):
        to = lax.rem(me + m, nfs)
        return pltpu.make_async_remote_copy(
            src_ref=sbuf.at[j, pl.ds(pl.multiple_of(to * rr, rr), rr), :],
            dst_ref=rbuf.at[m, j],
            send_sem=r_send.at[m, j],
            recv_sem=r_recv.at[m, j],
            device_id={"fs": to},
            device_id_type=MESH,
        )

    def project(j, side):
        sacc[...] = jnp.zeros_like(sacc)

        @pl.loop(0, tokens // tile)
        def _(t):
            rows = pl.ds(pl.multiple_of(t * tile, tile), tile)
            reduced = jnp.dot(xbuf[side, rows, :], pfull[j], preferred_element_type=F32)
            sacc[...] += lax.dot_general(
                reduced.astype(BF16), ybuf[j, rows, :], (((0,), (0,)), ((), ())), preferred_element_type=F32
            )

        sbuf[j] = sacc[...].astype(BF16)

    loads[1].wait()
    loads[2].wait()
    project(0, 0)
    weights[0].tick()
    weights[3].tick()
    for m in range(1, nfs):
        scatter_copy(0, m).start()
    weights[1].tick()
    loads[3].wait()
    project(1, 0)
    for m in range(1, nfs):
        scatter_copy(1, m).start()
    weights[0].tick()
    weights[1].tick()
    weights[3].tick()
    loads[4].wait()
    loads[5].wait()
    project(2, 1)
    for m in range(1, nfs):
        scatter_copy(2, m).start()
    weights[2].tick()
    weights[1].tick()
    weights[3].tick()

    squares = jnp.zeros((), F32)
    for j in range(3):
        value = sbuf[j, pl.ds(pl.multiple_of(me * rr, rr), rr), :].astype(F32)
        for m in range(1, nfs):
            scatter_copy(j, m).wait_recv()
            value = value + rbuf[m, j].astype(F32)
        fresh = 0.8 * m_ref[j] + 0.2 * value
        new_m[j] = fresh
        nmfull[j, pl.ds(pl.multiple_of(me * rr, rr), rr), :] = fresh.astype(BF16)
        squares = squares + jnp.sum(fresh * fresh)
    tbuf[0] = jnp.full(tbuf.shape[1:], squares, F32)

    def spread(buf, send, recv, axis, size, m):
        to = lax.rem(lax.axis_index(axis) + m, size)
        return pltpu.make_async_remote_copy(
            src_ref=buf.at[0],
            dst_ref=buf.at[m],
            send_sem=send.at[m],
            recv_sem=recv.at[m],
            device_id={axis: to},
            device_id_type=MESH,
        )

    momentum.tick()
    for m in range(1, nfs):
        spread(tbuf, t_send, t_recv, "fs", nfs, m).start()
    momentum.tick()
    part = tbuf[0]
    for m in range(1, nfs):
        spread(tbuf, t_send, t_recv, "fs", nfs, m).wait_recv()
        part = part + tbuf[m]
    ubuf[0] = part
    for m in range(1, ntp):
        spread(ubuf, u_send, u_recv, "tp", ntp, m).start()
    momentum.tick()
    weights[1].tick()
    weights[2].tick()
    momentum.tick()
    weights[3].tick()
    weights[2].tick()
    whole = part
    for m in range(1, ntp):
        spread(ubuf, u_send, u_recv, "tp", ntp, m).wait_recv()
        whole = whole + ubuf[m]
    total[...] = whole
    weights[2].tick()
    momentum.finish()
    for piece in weights:
        piece.finish()

    factors.drain()
    momentum.drain()
    for piece in weights:
        piece.drain()
    for m in range(1, nfs):
        owner = lax.rem(me + m, nfs)
        mate_copy(owner, core).wait_send()
        for j in range(3):
            scatter_copy(j, m).wait_send()
        spread(tbuf, t_send, t_recv, "fs", nfs, m).wait_send()
    for m in range(1, ntp):
        spread(ubuf, u_send, u_recv, "tp", ntp, m).wait_send()


def exchange(nfs, ntp, x, o, q, k, v, w16, p, m):
    block, rank = p.shape[1], p.shape[2]
    rr, cols = m.shape[1], m.shape[2]
    tokens, model = x.shape
    anywhere = pl.BlockSpec(memory_space=pl.ANY)
    vmem = pl.BlockSpec(memory_space=pltpu.VMEM)
    dma = pltpu.SemaphoreType.DMA
    return pl.pallas_call(
        functools.partial(exchange_kernel, nfs, ntp),
        out_shape=(
            jax.ShapeDtypeStruct((3, nfs * block, cols), BF16),
            jax.ShapeDtypeStruct((3, nfs * block, rank), BF16),
            jax.ShapeDtypeStruct((3, rank, cols), BF16),
            jax.ShapeDtypeStruct(m.shape, F32),
            jax.ShapeDtypeStruct((8, 128), F32),
        ),
        in_specs=[anywhere] * 7 + [vmem],
        out_specs=(anywhere, vmem, vmem, vmem, vmem),
        scratch_shapes=[
            pltpu.VMEM((2, tokens, model), BF16),
            pltpu.VMEM((3, tokens, cols), BF16),
            pltpu.VMEM((rank, cols), F32),
            pltpu.VMEM((3, rank, cols), BF16),
            pltpu.VMEM((nfs, 3, rr, cols), BF16),
            pltpu.VMEM((nfs, 8, 128), F32),
            pltpu.VMEM((ntp, 8, 128), F32),
            dma((6,)),
            dma((nfs, 4)), dma((nfs,)),
            dma((nfs,)), dma((nfs,)),
            dma((4, nfs, 4)), dma((4, nfs)),
            dma((nfs, 4)), dma((nfs,)),
            dma((nfs, 3)), dma((nfs, 3)),
            dma((nfs,)), dma((nfs,)),
            dma((ntp,)), dma((ntp,)),
        ],
        compiler_params=pltpu.CompilerParams(has_side_effects=True, vmem_limit_bytes=56 * 2**20),
        cost_estimate=pl.CostEstimate(flops=8 * 10**9, bytes_accessed=40 * 10**6, transcendentals=0),
        name="exchange",
    )(x, o, q, k, v, w16, p, m)


def update_kernel(nfs, entries, w_ref, p_ref, n_ref, t_ref, master_ref, m_ref, nw_ref, copies_ref, steps_ref, mo_ref):
    step_at = pl.program_id(0)
    me = lax.axis_index("fs")
    scale = 1.0 / jnp.sqrt(t_ref[0:1, 0:1] / entries + 1e-06)
    for j in range(3):
        step = jnp.dot(p_ref[j], n_ref[j], preferred_element_type=F32) * scale

        @pl.when(step_at == me)
        def _():
            steps_ref[j] = step
            fresh = master_ref[j] - 0.05 * step
            nw_ref[j] = fresh
            copies_ref[j] = fresh.astype(BF16)
            mo_ref[j] = m_ref[j]

        @pl.when(step_at != me)
        def _():
            copies_ref[j] = (w_ref[j].astype(F32) - 0.05 * step).astype(BF16)


def update(nfs, ntp, wfull, pfull, nmfull, total, master, new_m):
    block, cols = master.shape[1], master.shape[2]
    rank = nmfull.shape[1]
    entries = float(3 * rank * cols * ntp)
    whole = lambda a: pl.BlockSpec(a.shape, lambda b: (0,) * a.ndim)
    per_block = lambda width: pl.BlockSpec((3, block, width), lambda b: (0, b, 0))
    return pl.pallas_call(
        functools.partial(update_kernel, nfs, entries),
        grid=(nfs,),
        out_shape=(
            jax.ShapeDtypeStruct(master.shape, F32),
            jax.ShapeDtypeStruct(wfull.shape, BF16),
            jax.ShapeDtypeStruct(master.shape, F32),
            jax.ShapeDtypeStruct(new_m.shape, F32),
        ),
        in_specs=[per_block(cols), per_block(rank), whole(nmfull), whole(total), whole(master), whole(new_m)],
        out_specs=(whole(master), per_block(cols), whole(master), whole(new_m)),
        compiler_params=pltpu.CompilerParams(dimension_semantics=("arbitrary",)),
        cost_estimate=pl.CostEstimate(flops=2 * 10**9, bytes_accessed=20 * 10**6, transcendentals=0),
        name="update",
    )(wfull, pfull, nmfull, total, master, new_m)


def solution(mesh):
    nfs, ntp = mesh.shape["fs"], mesh.shape["tp"]

    def on_device(x, o, q, k, v, master, p, m):
        wfull, pfull, nmfull, new_m, total = exchange(nfs, ntp, x, o, q, k, v, master.astype(BF16), p, m)
        return update(nfs, ntp, wfull, pfull, nmfull, total, master, new_m)

    in_specs = (
        P("fs", None),
        P("fs", None),
        P("fs", "tp"),
        P("fs", "tp"),
        P("fs", "tp"),
        P(None, "fs", "tp"),
        P(None, "fs", None),
        P(None, "fs", "tp"),
    )
    out_specs = (P(None, "fs", "tp"), P(None, None, "tp"), P(None, "fs", "tp"), P(None, "fs", "tp"))
    return jax.shard_map(
        on_device, mesh=mesh, in_specs=in_specs, out_specs=out_specs, check_vma=False
    )
```

```python
import functools

import jax
import jax.numpy as jnp
from jax import lax
from jax.experimental import pallas as pl
from jax.experimental.pallas import tpu as pltpu
from jax.sharding import PartitionSpec as P

MESH = pl.DeviceIdType.MESH
F32 = jnp.float32
BF16 = jnp.bfloat16
PITCH = 0.5
PACE = (3, 3, 4, 6, 2, 2, 2, 2)


def grid_of(count):
    cols = 1
    while cols * cols * 4 <= count:
        cols *= 2
    return count // cols, cols


class Relay:
    def __init__(self, own, slot, send, recv, first, second, dev, hook=None, hook_drain=None):
        self.own, self.slot, self.send, self.recv = own, slot, send, recv
        (self.a, self.na), (self.b, self.nb) = first, second
        self.dev, self.hook, self.hook_drain = dev, hook, hook_drain
        a, b = self.a, self.b
        self.open = [a + 1 < self.na, a >= 1, b + 1 < self.nb, b >= 1]
        self.target = [(a + 1, b), (a - 1, b), (a, b + 1), (a, b - 1)]
        self.sent = []
        self.steps = [self.start]
        self.steps += [functools.partial(self.along_first, k) for k in range(1, self.na)]
        self.steps += [functools.partial(self.along_second, k) for k in range(1, self.nb)]
        self.at = 0

    def copy(self, owner, way, src):
        return pltpu.make_async_remote_copy(
            src_ref=src,
            dst_ref=self.slot(owner),
            send_sem=self.send.at[owner, way],
            recv_sem=self.recv.at[owner],
            device_id={"fs": self.dev(*self.target[way])},
            device_id_type=MESH,
        )

    def push(self, cond, owner, way, src):
        both = self.open[way] if cond is None else jnp.logical_and(cond, self.open[way])
        self.sent.append((both, owner, way, src))

        @pl.when(both)
        def _():
            self.copy(owner, way, src).start()

    def arrive(self, cond, owner, ways, came):
        @pl.when(cond)
        def _():
            self.copy(owner, came, self.slot(owner)).wait_recv()

        for way in ways:
            self.push(cond, owner, way, self.slot(owner))
        if self.hook is not None:

            @pl.when(cond)
            def _():
                self.hook(owner)

    def start(self):
        me = self.dev(self.a, self.b)
        for way in range(4):
            self.push(None, me, way, self.own)

    def along_first(self, k):
        self.arrive(self.a >= k, self.dev(self.a - k, self.b), (0, 2, 3), 1)
        self.arrive(self.a + k < self.na, self.dev(self.a + k, self.b), (1, 2, 3), 0)

    def along_second(self, k):
        for row in range(self.na):
            self.arrive(self.b >= k, self.dev(row, self.b - k), (2,), 3)
            self.arrive(self.b + k < self.nb, self.dev(row, self.b + k), (3,), 2)

    def tick(self, count=1):
        for _ in range(count):
            if self.at < len(self.steps):
                self.steps[self.at]()
                self.at += 1

    def finish(self):
        self.tick(len(self.steps))

    def drain(self):
        for cond, owner, way, src in self.sent:

            @pl.when(cond)
            def _():
                self.copy(owner, way, src).wait_send()


def exchange_kernel(
    nfs, ntp,
    x_in, o_in, q_in, k_in, v_in, w_in, p_in, m_ref,
    wfull, pfull, nmfull, new_m, total,
    xbuf, ybuf, wbuf, w16, sacc, sbuf, rbuf, tbuf, ubuf,
    load_sem, p_send, p_recv, d_send, d_recv, w_send, w_recv, n_send, n_recv,
    r_send, r_recv, t_send, t_recv, u_send, u_recv,
):
    me = lax.axis_index("fs")
    tp = lax.axis_index("tp")
    nz, nx = grid_of(nfs)
    z, x = me // nx, me % nx
    core = tp % 2
    mate = tp + 1 - 2 * core
    block = p_in.shape[1]
    half = block // 2
    rr = m_ref.shape[1]

    barrier = pltpu.get_barrier_semaphore()
    for m in range(1, nfs):
        pl.semaphore_signal(barrier, inc=1, device_id={"fs": lax.rem(me + m, nfs)}, device_id_type=MESH)
    for m in range(1, ntp):
        pl.semaphore_signal(barrier, inc=1, device_id={"tp": lax.rem(tp + m, ntp)}, device_id_type=MESH)

    loads = [
        pltpu.make_async_copy(p_in, pfull.at[:, pl.ds(pl.multiple_of(me * block, block), block), :], load_sem.at[0]),
        pltpu.make_async_copy(x_in, xbuf.at[0], load_sem.at[1]),
        pltpu.make_async_copy(q_in, ybuf.at[0], load_sem.at[2]),
        pltpu.make_async_copy(k_in, ybuf.at[1], load_sem.at[3]),
        pltpu.make_async_copy(o_in, xbuf.at[1], load_sem.at[4]),
        pltpu.make_async_copy(v_in, ybuf.at[2], load_sem.at[5]),
        pltpu.make_async_copy(w_in, wbuf, load_sem.at[6]),
    ]

    def zx(row, col):
        return row * nx + col

    def xz(col, row):
        return row * nx + col

    def p_slot(j, owner, which):
        return pfull.at[j, pl.ds(pl.multiple_of(owner * block + which * half, half), half), :]

    def mate_copy(j, owner, which):
        return pltpu.make_async_remote_copy(
            src_ref=p_slot(j, owner, which),
            dst_ref=p_slot(j, owner, which),
            send_sem=d_send.at[j, owner],
            recv_sem=d_recv.at[j, owner],
            device_id={"tp": mate},
            device_id_type=MESH,
        )

    def factor_piece(j):
        return Relay(
            p_in.at[j, pl.ds(pl.multiple_of(core * half, half), half), :],
            lambda owner: p_slot(j, owner, core),
            p_send.at[j], p_recv.at[j], (z, nz), (x, nx), zx,
            hook=lambda owner: mate_copy(j, owner, core).start(),
        )

    factors = [factor_piece(j) for j in range(3)]

    def w_piece(index, j, low, size, across):
        def slot(owner):
            return wfull.at[j, pl.ds(pl.multiple_of(owner * block + low, half), size), :]

        first, second, dev = ((x, nx), (z, nz), xz) if across else ((z, nz), (x, nx), zx)
        return Relay(
            w16.at[j, pl.ds(low, size), :], slot, w_send.at[index], w_recv.at[index], first, second, dev
        )

    weights = [
        w_piece(2 * j + h, j, h * half, half, 2 * j + h == 5) for j in range(3) for h in range(2)
    ]
    order = sorted(
        (stage + PITCH * index, index) for index, piece in enumerate(weights) for stage in range(len(piece.steps))
    )

    def carry(count):
        for _ in range(min(count, len(order))):
            weights[order.pop(0)[1]].tick()

    def n_slot(owner):
        return nmfull.at[:, pl.ds(pl.multiple_of(owner * rr, rr), rr), :]

    momentum = Relay(n_slot(me), n_slot, n_send, n_recv, (z, nz), (x, nx), zx)

    for load in loads:
        load.start()
    pl.semaphore_wait(barrier, nfs + ntp - 2)
    for piece in factors:
        piece.tick()
    loads[6].wait()
    w16[...] = wbuf[...].astype(BF16)
    for _ in range(nz - 2):
        for piece in factors:
            piece.tick()
    factors[0].tick()
    factors[1].tick()
    carry(PACE[0])

    tokens = xbuf.shape[1]
    tile = min(256, tokens)

    def scatter_copy(j, m):
        to = lax.rem(me + m, nfs)
        return pltpu.make_async_remote_copy(
            src_ref=sbuf.at[j, pl.ds(pl.multiple_of(to * rr, rr), rr), :],
            dst_ref=rbuf.at[m, j],
            send_sem=r_send.at[m, j],
            recv_sem=r_recv.at[m, j],
            device_id={"fs": to},
            device_id_type=MESH,
        )

    def project(j, side):
        sacc[...] = jnp.zeros_like(sacc)

        @pl.loop(0, tokens // tile)
        def _(t):
            rows = pl.ds(pl.multiple_of(t * tile, tile), tile)
            reduced = jnp.dot(xbuf[side, rows, :], pfull[j], preferred_element_type=F32)
            sacc[...] += lax.dot_general(
                reduced.astype(BF16), ybuf[j, rows, :], (((0,), (0,)), ((), ())), preferred_element_type=F32
            )

        sbuf[j] = sacc[...].astype(BF16)

    def ready(j):
        factors[j].finish()
        for m in range(1, nfs):
            mate_copy(j, lax.rem(me + m, nfs), 1 - core).wait_recv()

    def scatter(j):
        for m in range(1, nfs):
            scatter_copy(j, m).start()

    loads[0].wait()
    loads[1].wait()
    loads[2].wait()
    ready(0)
    project(0, 0)
    scatter(0)
    factors[2].tick()
    carry(PACE[1])
    loads[3].wait()
    ready(1)
    project(1, 0)
    scatter(1)
    carry(PACE[2])
    loads[4].wait()
    loads[5].wait()
    ready(2)
    project(2, 1)
    scatter(2)
    carry(PACE[3])

    squares = jnp.zeros((), F32)
    for j in range(3):
        value = sbuf[j, pl.ds(pl.multiple_of(me * rr, rr), rr), :].astype(F32)
        for m in range(1, nfs):
            scatter_copy(j, m).wait_recv()
            value = value + rbuf[m, j].astype(F32)
        fresh = 0.8 * m_ref[j] + 0.2 * value
        new_m[j] = fresh
        nmfull[j, pl.ds(pl.multiple_of(me * rr, rr), rr), :] = fresh.astype(BF16)
        squares = squares + jnp.sum(fresh * fresh)
    tbuf[0] = jnp.full(tbuf.shape[1:], squares, F32)

    def spread(buf, send, recv, axis, size, m):
        to = lax.rem(lax.axis_index(axis) + m, size)
        return pltpu.make_async_remote_copy(
            src_ref=buf.at[0],
            dst_ref=buf.at[m],
            send_sem=send.at[m],
            recv_sem=recv.at[m],
            device_id={axis: to},
            device_id_type=MESH,
        )

    momentum.tick()
    for m in range(1, nfs):
        spread(tbuf, t_send, t_recv, "fs", nfs, m).start()
    carry(PACE[4])
    momentum.tick()
    carry(PACE[5])
    momentum.tick()
    part = tbuf[0]
    for m in range(1, nfs):
        spread(tbuf, t_send, t_recv, "fs", nfs, m).wait_recv()
        part = part + tbuf[m]
    ubuf[0] = part
    for m in range(1, ntp):
        spread(ubuf, u_send, u_recv, "tp", ntp, m).start()
    carry(PACE[6])
    momentum.tick()
    carry(PACE[7])
    whole = part
    for m in range(1, ntp):
        spread(ubuf, u_send, u_recv, "tp", ntp, m).wait_recv()
        whole = whole + ubuf[m]
    total[...] = whole
    momentum.finish()
    carry(len(order))

    for piece in factors:
        piece.drain()
    momentum.drain()
    for piece in weights:
        piece.drain()
    for m in range(1, nfs):
        owner = lax.rem(me + m, nfs)
        for j in range(3):
            mate_copy(j, owner, core).wait_send()
            scatter_copy(j, m).wait_send()
        spread(tbuf, t_send, t_recv, "fs", nfs, m).wait_send()
    for m in range(1, ntp):
        spread(ubuf, u_send, u_recv, "tp", ntp, m).wait_send()


def exchange(nfs, ntp, x, o, q, k, v, w, p, m):
    block, rank = p.shape[1], p.shape[2]
    rr, cols = m.shape[1], m.shape[2]
    tokens, model = x.shape
    anywhere = pl.BlockSpec(memory_space=pl.ANY)
    vmem = pl.BlockSpec(memory_space=pltpu.VMEM)
    dma = pltpu.SemaphoreType.DMA
    return pl.pallas_call(
        functools.partial(exchange_kernel, nfs, ntp),
        out_shape=(
            jax.ShapeDtypeStruct((3, nfs * block, cols), BF16),
            jax.ShapeDtypeStruct((3, nfs * block, rank), BF16),
            jax.ShapeDtypeStruct((3, rank, cols), BF16),
            jax.ShapeDtypeStruct(m.shape, F32),
            jax.ShapeDtypeStruct((8, 128), F32),
        ),
        in_specs=[anywhere] * 7 + [vmem],
        out_specs=(anywhere, vmem, vmem, vmem, vmem),
        scratch_shapes=[
            pltpu.VMEM((2, tokens, model), BF16),
            pltpu.VMEM((3, tokens, cols), BF16),
            pltpu.VMEM(w.shape, F32),
            pltpu.VMEM(w.shape, BF16),
            pltpu.VMEM((rank, cols), F32),
            pltpu.VMEM((3, rank, cols), BF16),
            pltpu.VMEM((nfs, 3, rr, cols), BF16),
            pltpu.VMEM((nfs, 8, 128), F32),
            pltpu.VMEM((ntp, 8, 128), F32),
            dma((7,)),
            dma((3, nfs, 4)), dma((3, nfs)),
            dma((3, nfs)), dma((3, nfs)),
            dma((6, nfs, 4)), dma((6, nfs)),
            dma((nfs, 4)), dma((nfs,)),
            dma((nfs, 3)), dma((nfs, 3)),
            dma((nfs,)), dma((nfs,)),
            dma((ntp,)), dma((ntp,)),
        ],
        compiler_params=pltpu.CompilerParams(collective_id=0, has_side_effects=True, vmem_limit_bytes=56 * 2**20),
        cost_estimate=pl.CostEstimate(flops=8 * 10**9, bytes_accessed=40 * 10**6, transcendentals=0),
        name="exchange",
    )(x, o, q, k, v, w, p, m)


def update_kernel(nfs, entries, w_ref, p_ref, n_ref, t_ref, master_ref, m_ref, nw_ref, copies_ref, steps_ref, mo_ref):
    step_at = pl.program_id(0)
    me = lax.axis_index("fs")
    scale = 1.0 / jnp.sqrt(t_ref[0:1, 0:1] / entries + 1e-06)
    for j in range(3):
        step = jnp.dot(p_ref[j], n_ref[j], preferred_element_type=F32) * scale

        @pl.when(step_at == me)
        def _():
            steps_ref[j] = step
            fresh = master_ref[j] - 0.05 * step
            nw_ref[j] = fresh
            copies_ref[j] = fresh.astype(BF16)
            mo_ref[j] = m_ref[j]

        @pl.when(step_at != me)
        def _():
            copies_ref[j] = (w_ref[j].astype(F32) - 0.05 * step).astype(BF16)


def update(nfs, ntp, wfull, pfull, nmfull, total, master, new_m):
    block, cols = master.shape[1], master.shape[2]
    rank = nmfull.shape[1]
    entries = float(3 * rank * cols * ntp)
    whole = lambda a: pl.BlockSpec(a.shape, lambda b: (0,) * a.ndim)
    per_block = lambda width: pl.BlockSpec((3, block, width), lambda b: (0, b, 0))
    return pl.pallas_call(
        functools.partial(update_kernel, nfs, entries),
        grid=(nfs,),
        out_shape=(
            jax.ShapeDtypeStruct(master.shape, F32),
            jax.ShapeDtypeStruct(wfull.shape, BF16),
            jax.ShapeDtypeStruct(master.shape, F32),
            jax.ShapeDtypeStruct(new_m.shape, F32),
        ),
        in_specs=[per_block(cols), per_block(rank), whole(nmfull), whole(total), whole(master), whole(new_m)],
        out_specs=(whole(master), per_block(cols), whole(master), whole(new_m)),
        compiler_params=pltpu.CompilerParams(dimension_semantics=("arbitrary",)),
        cost_estimate=pl.CostEstimate(flops=2 * 10**9, bytes_accessed=20 * 10**6, transcendentals=0),
        name="update",
    )(wfull, pfull, nmfull, total, master, new_m)


def solution(mesh):
    nfs, ntp = mesh.shape["fs"], mesh.shape["tp"]

    def on_device(x, o, q, k, v, master, p, m):
        wfull, pfull, nmfull, new_m, total = exchange(nfs, ntp, x, o, q, k, v, master, p, m)
        return update(nfs, ntp, wfull, pfull, nmfull, total, master, new_m)

    in_specs = (
        P("fs", None),
        P("fs", None),
        P("fs", "tp"),
        P("fs", "tp"),
        P("fs", "tp"),
        P(None, "fs", "tp"),
        P(None, "fs", None),
        P(None, "fs", "tp"),
    )
    out_specs = (P(None, "fs", "tp"), P(None, None, "tp"), P(None, "fs", "tp"), P(None, "fs", "tp"))
    return jax.shard_map(
        on_device, mesh=mesh, in_specs=in_specs, out_specs=out_specs, check_vma=False
    )
```
